512 devices in a mesh: sp: 64 (over z, y), fs: 4 (over x), tp: 2 (over core).
Axes of the slice: x: 4, y: 8, z: 8, core: 2. Of those that a mesh axis runs over, the one named last changes fastest.
Arguments:
- recurrent_query: bfloat16 [4, 16384, 1024], P('fs', 'sp', 'tp'), may hold values from -6 to 6
- forget_logits: bfloat16 [4, 16384, 1024], P('fs', 'sp', 'tp'), may hold values from -6 to 6
- recurrent_value: bfloat16 [4, 16384, 1024], P('fs', 'sp', 'tp'), may hold values from -6 to 6
- forget_floor: float32 [2, 1024], P(None, 'tp'), may hold values from 0.8 to 1
- extra_log_decay: float32 [4, 16384, 8], P('fs', 'sp', 'tp'), may hold values from -1 to 0
- recurrent_norm_gain: float32 [1024], P('tp'), may hold values from 0.1 to 1.9
- attention_query: bfloat16 [4, 16384, 768], P('fs', 'sp', 'tp'), may hold values from -300 to 300
- latent: bfloat16 [4, 16384, 256], P('fs', 'sp'), may hold values from -6 to 6
- rotary_key: bfloat16 [4, 16384, 32], P('fs', 'sp'), may hold values from -15 to 15
- latent_norm_gain: float32 [256], replicated, may hold values from 0.1 to 1.9
- latent_up_weight: bfloat16 [256, 1024], replicated, may hold values from -0.375 to 0.375
- recurrent_output_weight: bfloat16 [1024, 2048], P('tp', 'fs'), may hold values from -0.1875 to 0.1875
- attention_output_weight: bfloat16 [512, 2048], P('tp', 'fs'), may hold values from -2 to 2
Outputs:
- mixed: bfloat16 [4, 16384, 2048], P('fs', ('sp', 'tp'))
- log_weight: float32 [4, 16384, 8], P('fs', 'sp', 'tp')
The draws below stay inside these ranges and needn't reach their ends.
All inputs are finite; a program needn't handle non-finite values.
Results may differ from the reference program's by a relative error of at most 0.013.
The reference program's roundings to bfloat16 on the way count: a program that leaves them out, or rounds other values in their place, can miss the bound.
Values may be sent and summed in bfloat16 or wider, within the bound.
No kernel may reach another device: no remote copies, remote signals or barrier semaphores. Data moves between devices by JAX's collectives and lax.ppermute only.
A program may use at most 128 MiB of HBM per device.

```python
import math
import jax
import jax.numpy as jnp
from jax import lax

D = 2048
RECURRENT_HEADS = 8
HG_DK = 128
HG_DV = 128
MLA_HEADS = 8
NOPE = 64
ROPE = 32
VDIM = 64
KV_RANK = 256
HG_BLOCK = 64
TOK_DEV = 256
SEQUENCE_LENGTH = 2048
SEQUENCE_GROUPS = 4
GROUP_TOKENS = 16384
HG_KEY = 1024
HG_WIDTH = 1024
MLA_WIDTH = 512
N_TP = 2


def draw_forget_floor(key, part):
    pick_key, fast_key, rate_key = jax.random.split(jax.random.fold_in(key, 1), 3)
    slow_share = 0.5
    slowly = jax.random.uniform(pick_key, (2, RECURRENT_HEADS, 1), jnp.float32) < slow_share
    fast_bound = jax.random.uniform(fast_key, (2, RECURRENT_HEADS, HG_DK), jnp.float32, 0.8, 0.92)
    slow_rates = jnp.exp(jax.random.uniform(rate_key, (2, RECURRENT_HEADS, HG_DK), jnp.float32, math.log(0.02), math.log(0.08))) / SEQUENCE_LENGTH
    bounds = jnp.where(slowly, 1.0 - slow_rates, fast_bound)
    return bounds.reshape(2, HG_KEY).astype(jnp.float32)


def draw_extra_log_decay(key, part):
    level_key, striking_key, falling_key = jax.random.split(jax.random.fold_in(key, 2), 3)
    blocks = GROUP_TOKENS // TOK_DEV
    levels = jnp.exp(jax.random.uniform(level_key, (SEQUENCE_GROUPS, blocks, 1, RECURRENT_HEADS), jnp.float32, math.log(0.15), math.log(0.6))) / SEQUENCE_LENGTH
    stable_value = -jnp.broadcast_to(levels, (SEQUENCE_GROUPS, blocks, TOK_DEV, RECURRENT_HEADS)).reshape(SEQUENCE_GROUPS, GROUP_TOKENS, RECURRENT_HEADS)
    spike_strikes = jax.random.uniform(striking_key, (SEQUENCE_GROUPS, GROUP_TOKENS, RECURRENT_HEADS), jnp.float32) < 2.0 / SEQUENCE_LENGTH
    spike_falls = jnp.log(jax.random.uniform(falling_key, (SEQUENCE_GROUPS, GROUP_TOKENS, RECURRENT_HEADS), jnp.float32, 0.5, 0.8))
    return (stable_value + jnp.where(spike_strikes, spike_falls, 0.0)).astype(jnp.float32)


def drawn_keys(key):
    base_keys = jnp.clip(jax.random.normal(jax.random.fold_in(key, 5), (SEQUENCE_GROUPS, GROUP_TOKENS, ROPE), jnp.float32), -4.5, 4.5)
    return base_keys


def draw_rotary_key(key, part):
    base_keys = drawn_keys(key)
    values = base_keys
    return values.astype(jnp.bfloat16)


def draw_attention_query(key, part):
    normal = jnp.clip(2.0 * jax.random.normal(jax.random.fold_in(key, 6), (SEQUENCE_GROUPS, GROUP_TOKENS, MLA_HEADS, NOPE + ROPE), jnp.float32), -12.0, 12.0)
    return normal.reshape(SEQUENCE_GROUPS, GROUP_TOKENS, MLA_HEADS * (NOPE + ROPE)).astype(jnp.bfloat16)


def block_levels(key, extent, pieces, least, largest):
    loudness = 1.0
    for axis_at, shards_of in pieces:
        steps = jax.random.uniform(jax.random.fold_in(jax.random.fold_in(key, 6), axis_at), (shards_of,), jnp.float32, least / len(pieces), largest / len(pieces))
        loudness = loudness * jnp.repeat(jnp.exp(steps), extent[axis_at] // shards_of).reshape((-1,) + (1,) * (len(extent) - 1 - axis_at))
    return loudness


def gaussian(own_key, dims, deviation, limit, pieces=(), kind=jnp.bfloat16):
    entries = jax.random.normal(own_key, dims, jnp.float32) * deviation
    if len(pieces) > 0:
        entries = block_levels(own_key, dims, pieces, -0.22, 0.18) * entries
    return jnp.clip(entries, min=-limit, max=limit).astype(kind)


def setup_inputs(seed: int = 0) -> dict:
    key_of = jax.random.split(jax.random.key(seed), 14)
    recurrent_query = gaussian(key_of[0], (SEQUENCE_GROUPS, GROUP_TOKENS, HG_KEY), 1.0, 6.0, ((0, 4), (1, 64), (2, 2)))
    forget_logits = gaussian(key_of[1], (SEQUENCE_GROUPS, GROUP_TOKENS, HG_KEY), 1.0, 6.0, ((0, 4), (1, 64), (2, 2)))
    recurrent_value = gaussian(key_of[2], (SEQUENCE_GROUPS, GROUP_TOKENS, HG_WIDTH), 1.0, 6.0, ((0, 4), (1, 64), (2, 2)))
    forget_floor = draw_forget_floor(jax.random.fold_in(key_of[13], 71), 0)
    extra_log_decay = draw_extra_log_decay(jax.random.fold_in(key_of[13], 71), 0)
    recurrent_norm_gain = jnp.clip(1.0 + 0.18 * jax.random.normal(key_of[5], (HG_WIDTH,), jnp.float32), 0.1, 1.9)
    attention_query = draw_attention_query(jax.random.fold_in(key_of[13], 71), 0)
    latent = gaussian(key_of[7], (SEQUENCE_GROUPS, GROUP_TOKENS, KV_RANK), 1.0, 6.0, ((0, 4), (1, 64)))
    rotary_key = draw_rotary_key(jax.random.fold_in(key_of[13], 71), 0)
    latent_norm_gain = jnp.clip(1.0 + 0.18 * jax.random.normal(key_of[9], (KV_RANK,), jnp.float32), 0.1, 1.9)
    latent_up_weight = gaussian(key_of[10], (KV_RANK, MLA_HEADS * (NOPE + VDIM)), KV_RANK ** -0.5, 0.375)
    recurrent_output_weight = gaussian(key_of[11], (HG_WIDTH, D), HG_WIDTH ** -0.5, 0.1875, ((0, 2), (1, 4)))
    attention_output_weight = gaussian(key_of[12], (MLA_WIDTH, D), (max(MLA_WIDTH // 64, 1)) ** -0.5, 2.0, ((0, 2), (1, 4)))
    return dict(recurrent_query=recurrent_query, forget_logits=forget_logits, recurrent_value=recurrent_value, forget_floor=forget_floor, extra_log_decay=extra_log_decay, recurrent_norm_gain=recurrent_norm_gain, attention_query=attention_query, latent=latent, rotary_key=rotary_key, latent_norm_gain=latent_norm_gain, latent_up_weight=latent_up_weight, recurrent_output_weight=recurrent_output_weight, attention_output_weight=attention_output_weight)


norm_eps = 1e-06
rope_base = 10000.0
largest_value = lax.Precision.HIGHEST

def rope_tables(token_count, offset):
    places = offset + jnp.arange(token_count).astype(jnp.float32)
    pair_count = ROPE // 2
    inverse = rope_base ** (-jnp.arange(pair_count).astype(jnp.float32) / pair_count)
    angles = places[:, None] * inverse[None, :]
    return (jnp.cos(angles), jnp.sin(angles))

def rotate(tensor, cos_table, sin_table):
    half_width = tensor.shape[-1] // 2
    first_half = tensor[..., :half_width]
    second_half = tensor[..., half_width:]
    return jnp.concatenate([first_half * cos_table - second_half * sin_table, first_half * sin_table + second_half * cos_table], axis=-1)

def block_pass(queries, key_matrix, values, decay_logarithm, carried):
    length = queries.shape[0]
    blocks = length // HG_BLOCK

    def split_blocks(tensor):
        return tensor.reshape((blocks, HG_BLOCK) + tensor.shape[1:])
    lower_mask = jnp.tril(jnp.ones((HG_BLOCK, HG_BLOCK), dtype=bool))

    def advance(running_state, input_tuple):
        query_blk, key_tile, value_tile, decay_blk = input_tuple
        inner_block_term = jnp.cumsum(decay_blk, axis=0)
        damped_query = query_blk * jnp.exp(inner_block_term)
        key_decayed = key_tile * jnp.exp(-inner_block_term)
        cross_block_term = jnp.einsum('mcx,cxn->mcn', damped_query, running_state, precision=largest_value)
        scores = jnp.einsum('thk,shk->hts', damped_query, key_decayed, precision=largest_value)
        scores = jnp.where(lower_mask[None], scores, 0.0)
        intra_term = jnp.einsum('hts,shv->thv', scores, value_tile, precision=largest_value)
        decay_total = inner_block_term[-1]
        updated_state = jnp.exp(decay_total)[:, :, None] * running_state + jnp.einsum('jrg,jrb->rgb', key_tile * jnp.exp(decay_total[None] - inner_block_term), value_tile, precision=largest_value)
        return (updated_state, cross_block_term + intra_term)
    final_state, outputs = lax.scan(advance, carried, (split_blocks(queries), split_blocks(key_matrix), split_blocks(values), split_blocks(decay_logarithm)))
    return (outputs.reshape((length,) + outputs.shape[2:]), final_state)

def gate_factors(forget_gate, spike_amount, gate_floor):
    decay_logarithm = jnp.logaddexp(jnp.log(gate_floor), jnp.log1p(-gate_floor) + jax.nn.log_sigmoid(forget_gate)) + spike_amount[:, :, None]
    key_matrix = (1.0 - gate_floor) * jax.nn.sigmoid(-forget_gate)
    return (key_matrix, decay_logarithm)

def head_norm(outputs, gain):
    return outputs * lax.rsqrt(lax.optimization_barrier(jnp.mean(outputs * outputs, axis=-1, keepdims=True)) + norm_eps) * gain

def recurrence_path(query_rows, forget_input, value_input, spike_amount, forget_floor, recurrent_norm_gain):
    length = query_rows.shape[0]
    queries = query_rows.astype(jnp.float32).reshape(length, RECURRENT_HEADS, HG_DK)
    forget_gate = forget_input.astype(jnp.float32).reshape(length, RECURRENT_HEADS, HG_DK)
    values = value_input.astype(jnp.float32).reshape(length, RECURRENT_HEADS, HG_DV)
    summed = jnp.zeros((length, RECURRENT_HEADS, HG_DV), jnp.float32)
    for direction in range(2):
        gate_floor = forget_floor[direction].reshape(RECURRENT_HEADS, HG_DK)
        key_matrix, decay_logarithm = gate_factors(forget_gate, spike_amount, gate_floor)
        sorted_rows = [queries, key_matrix, values, decay_logarithm]
        if direction == 1:
            sorted_rows = [jnp.flip(member, axis=0) for member in sorted_rows]
        result, unused = block_pass(sorted_rows[0], sorted_rows[1], sorted_rows[2], sorted_rows[3], jnp.zeros((RECURRENT_HEADS, HG_DK, HG_DV), jnp.float32))
        if direction == 1:
            result = jnp.flip(result, axis=0)
        summed = summed + result
    normed = head_norm(summed, recurrent_norm_gain.reshape(RECURRENT_HEADS, HG_DV))
    return normed.astype(jnp.bfloat16).reshape(length, RECURRENT_HEADS * HG_DV)

def attention_branch(query_rows, latent, rotary_key, latent_norm_gain, latent_up_weight):
    length = query_rows.shape[0]
    latent_wide = latent.astype(jnp.float32)
    normed = (latent_wide * lax.rsqrt(lax.optimization_barrier(jnp.mean(latent_wide * latent_wide, axis=-1, keepdims=True)) + norm_eps) * latent_norm_gain).astype(jnp.bfloat16)
    expanded = jnp.dot(normed, latent_up_weight, preferred_element_type=jnp.float32).astype(jnp.bfloat16)
    expanded = expanded.reshape(length, MLA_HEADS, NOPE + VDIM)
    cos_table, sin_table = rope_tables(length, 0.0)
    rotated_key = rotate(rotary_key.astype(jnp.float32), cos_table, sin_table).astype(jnp.bfloat16)
    head_query = query_rows.reshape(length, MLA_HEADS, NOPE + ROPE)
    query_rope = rotate(head_query[..., NOPE:].astype(jnp.float32), cos_table[:, None], sin_table[:, None])
    query_all = jnp.concatenate([head_query[..., :NOPE], query_rope.astype(jnp.bfloat16)], axis=-1)
    keys_all = jnp.concatenate([expanded[..., :NOPE], jnp.broadcast_to(rotated_key[:, None, :], (length, MLA_HEADS, ROPE))], axis=-1)
    values = expanded[..., NOPE:].astype(jnp.float32)
    keys_wide = keys_all.astype(jnp.float32)
    score_scale = (NOPE + ROPE) ** (-0.5)
    rows_block = min(length, 512)

    def one_block(query_block):
        scores = jnp.einsum('qhd,khd->hqk', query_block.astype(jnp.float32), keys_wide) * score_scale
        row_peak = lax.optimization_barrier(jnp.max(scores, axis=-1))
        weights = jnp.exp(scores - row_peak[..., None])
        totals = lax.optimization_barrier(jnp.sum(weights, axis=-1))
        rounded = lax.optimization_barrier(weights.astype(jnp.bfloat16)).astype(jnp.float32)
        weighted = jnp.einsum('hqk,khv->qhv', rounded, values) / totals.T[:, :, None]
        return (weighted.astype(jnp.bfloat16).reshape(rows_block, MLA_HEADS * VDIM), (row_peak + jnp.log(totals)).T)
    outputs, log_weight = lax.map(one_block, query_all.reshape(length // rows_block, rows_block, MLA_HEADS, NOPE + ROPE))
    return (outputs.reshape(length, MLA_HEADS * VDIM), log_weight.reshape(length, MLA_HEADS))

def reference(recurrent_query, forget_logits, recurrent_value, forget_floor, extra_log_decay, recurrent_norm_gain, attention_query, latent, rotary_key, latent_norm_gain, latent_up_weight, recurrent_output_weight, attention_output_weight):
    seq_count = SEQUENCE_GROUPS * (GROUP_TOKENS // SEQUENCE_LENGTH)

    def sequence_view(tensor):
        return tensor.reshape(seq_count, SEQUENCE_LENGTH, tensor.shape[-1])
    recurrence_result = lax.map(lambda input_tuple: recurrence_path(input_tuple[0], input_tuple[1], input_tuple[2], input_tuple[3], forget_floor, recurrent_norm_gain), (sequence_view(recurrent_query), sequence_view(forget_logits), sequence_view(recurrent_value), sequence_view(extra_log_decay)))
    attended, log_weight = lax.map(lambda input_tuple: attention_branch(input_tuple[0], input_tuple[1], input_tuple[2], latent_norm_gain, latent_up_weight), (sequence_view(attention_query), sequence_view(latent), sequence_view(rotary_key)))
    rows_total = SEQUENCE_GROUPS * GROUP_TOKENS
    recurrence_result = recurrence_result.reshape(rows_total, HG_WIDTH)
    attended = attended.reshape(rows_total, MLA_WIDTH)
    hg_share = HG_WIDTH // N_TP
    att_share = MLA_WIDTH // N_TP
    summed = jnp.zeros((rows_total, D), jnp.float32)
    for tp_half in range(N_TP):
        partial_term = jnp.dot(recurrence_result[:, tp_half * hg_share:(tp_half + 1) * hg_share], recurrent_output_weight[tp_half * hg_share:(tp_half + 1) * hg_share], preferred_element_type=jnp.float32)
        partial_term = partial_term + jnp.dot(attended[:, tp_half * att_share:(tp_half + 1) * att_share], attention_output_weight[tp_half * att_share:(tp_half + 1) * att_share], preferred_element_type=jnp.float32)
        summed = summed + lax.optimization_barrier(partial_term.astype(jnp.bfloat16)).astype(jnp.float32)
    mixed = summed.astype(jnp.bfloat16).reshape(SEQUENCE_GROUPS, GROUP_TOKENS, D)
    return (mixed, log_weight.reshape(SEQUENCE_GROUPS, GROUP_TOKENS, MLA_HEADS))
```

```python
import numpy as np

import jax
import jax.numpy as jnp
from jax import lax
from jax.experimental import pallas as pl
from jax.experimental.pallas import tpu as pltpu
from jax.sharding import Mesh
from jax.sharding import PartitionSpec as P

DK = 128
HEADS = 4
NOPE = 64
ROPE = 32
RANK = 256
BLOCK = 64
TOK = 256
HALF = 128
SEQ_DEV = 8
STATE_ROWS = 144
KV_ROWS = 288
CHUNK_ROWS = STATE_ROWS + KV_ROWS
SP = ("sp_0", "sp_1")
SP_TP = ("sp_0", "sp_1", "tp")
EPS = 1e-06
ROPE_BASE = 10000.0
SCALE = (NOPE + ROPE) ** (-0.5)
LOG2E = 1.4426950408889634

f32 = jnp.float32
bf16 = jnp.bfloat16
NT = (((1,), (1,)), ((), ()))
TN = (((0,), (0,)), ((), ()))


def dot(a, b, dims=(((1,), (0,)), ((), ()))):
    return lax.dot_general(a, b, dims, preferred_element_type=f32)


def iota2(shape, axis):
    return lax.broadcasted_iota(jnp.int32, shape, axis)


def exact_sum(selector, values):
    high = values.astype(bf16)
    rest = values - high.astype(f32)
    middle = rest.astype(bf16)
    low = (rest - middle.astype(f32)).astype(bf16)
    return dot(selector, high) + dot(selector, middle) + dot(selector, low)


def gate(logit, floor, extra):
    keyed = (1.0 - floor) * logit
    return keyed, jnp.log(1.0 - keyed) + extra


def head_extra(extra_ref, first, count):
    return jnp.concatenate(
        [
            jnp.broadcast_to(extra_ref[:, h : h + 1], (TOK, DK))
            for h in range(first, first + count)
        ],
        axis=1,
    )


def rotated(x, cos_table, sin_table):
    lane = iota2(x.shape, 1)
    partner = jnp.where(lane < NOPE + ROPE // 2, pltpu.roll(x, 128 - 16, 1), pltpu.roll(x, 16, 1))
    return x * cos_table + partner * sin_table


def send_kernel(
    tp_ref, logit_ref, value_ref, floor_ref, extra_ref, lat_ref, gain_ref, key_ref, cos_ref, sin_ref, out_ref
):
    rows = iota2((TOK, TOK), 0)
    cols = iota2((TOK, TOK), 1)
    after = (cols > rows).astype(f32).astype(bf16)
    before = (cols < rows).astype(f32).astype(bf16)
    for pair in range(HEADS // 2):
        lanes = slice(pair * 2 * DK, (pair + 1) * 2 * DK)
        closed = jax.nn.sigmoid(-logit_ref[:, lanes].astype(f32))
        extra = head_extra(extra_ref, 2 * pair, 2)
        for d in range(2):
            keyed, decay = gate(closed, floor_ref[d : d + 1, lanes], extra)
            left = exact_sum(after if d == 0 else before, decay)
            edge = 0 if d == 0 else TOK - 1
            total = jnp.exp(left[edge : edge + 1] + decay[edge : edge + 1])
            weighted = (keyed * jnp.exp(left)).astype(bf16)
            for s in range(2):
                h = 2 * pair + s
                state = dot(
                    value_ref[:, h * DK : (h + 1) * DK], weighted[:, s * DK : (s + 1) * DK], TN
                )
                out_ref[d * HEADS + h, 0:DK, :] = state.astype(bf16)
                out_ref[d * HEADS + h, DK:STATE_ROWS, :] = jnp.broadcast_to(
                    total[:, s * DK : (s + 1) * DK], (STATE_ROWS - DK, DK)
                ).astype(bf16)
    mine = pl.ds(pl.multiple_of(tp_ref[0] * HALF, HALF), HALF)
    wide = lat_ref[mine, :].astype(f32)
    mean = jnp.sum(wide * wide, axis=1, keepdims=True) * (1.0 / RANK)
    normed = (wide * lax.rsqrt(mean + EPS) * gain_ref[...]).astype(bf16)
    turned = rotated(key_ref[mine, :].astype(f32), cos_ref[mine, :], sin_ref[mine, :])
    lane = iota2((32, 128), 1)
    packed = jnp.zeros((32, 128), f32)
    for g in range(4):
        piece = pltpu.roll(turned[32 * g : 32 * g + 32], (32 * g - NOPE) % 128, 1)
        packed = jnp.where((lane >= 32 * g) & (lane < 32 * g + 32), piece, packed)
    packed = packed.astype(bf16)
    for q in range(SEQ_DEV):
        out_ref[q, STATE_ROWS : STATE_ROWS + 128, :] = normed[:, :128]
        out_ref[q, STATE_ROWS + 128 : STATE_ROWS + 256, :] = normed[:, 128:]
        out_ref[q, STATE_ROWS + 256 : CHUNK_ROWS, :] = packed


def local_kernel(query_ref, logit_ref, value_ref, floor_ref, extra_ref, out_ref, damped_ref):
    rows = iota2((TOK, TOK), 0)
    cols = iota2((TOK, TOK), 1)
    same = (rows // BLOCK) == (cols // BLOCK)
    lower = same & (cols <= rows)
    upper = same & (cols >= rows)
    blocks = TOK // BLOCK
    for h in range(HEADS):
        lanes = slice(h * DK, (h + 1) * DK)
        closed = jax.nn.sigmoid(-logit_ref[:, lanes].astype(f32))
        extra = head_extra(extra_ref, h, 1)
        query = query_ref[:, lanes].astype(f32)
        value = value_ref[:, lanes]
        outs = [None] * blocks
        inner_sum = jnp.zeros((TOK, DK), f32)
        for d in range(2):
            seen = lower if d == 0 else upper
            keyed, decay = gate(closed, floor_ref[d : d + 1, lanes], extra)
            within = exact_sum(seen.astype(f32).astype(bf16), decay)
            damped = query * jnp.exp(within)
            grown = (keyed * jnp.exp(-within)).astype(bf16)
            damped16 = damped.astype(bf16)
            scores = jnp.where(seen, dot(damped16, grown, NT), 0.0).astype(bf16)
            inner_sum = inner_sum + dot(scores, value)
            state = None
            offset = jnp.zeros((1, DK), f32)
            for b in range(blocks) if d == 0 else reversed(range(blocks)):
                at = slice(b * BLOCK, (b + 1) * BLOCK)
                edge = (b + 1) * BLOCK - 1 if d == 0 else b * BLOCK
                total = within[edge : edge + 1]
                damped_ref[d, at, lanes] = (damped[at] * jnp.exp(offset)).astype(bf16)
                if state is not None:
                    cross = dot(damped16[at], state.astype(bf16), NT)
                    outs[b] = cross if outs[b] is None else outs[b] + cross
                offset = offset + total
                if b == (blocks - 1 if d == 0 else 0):
                    continue
                weighted = (keyed[at] * jnp.exp(total - within[at])).astype(bf16)
                added = dot(value[at], weighted, TN)
                state = added if state is None else state * jnp.exp(total) + added
        for b in range(blocks):
            at = slice(b * BLOCK, (b + 1) * BLOCK)
            out_ref[at, lanes] = inner_sum[at] if outs[b] is None else inner_sum[at] + outs[b]


def scan_kernel(dir_ref, got_ref, out_ref):
    d = dir_ref[0]
    carried = jnp.zeros((DK, DK), f32)
    for k in range(SEQ_DEV):
        j = jnp.where(d == 0, k, SEQ_DEV - 1 - k)
        out_ref[j] = carried.astype(bf16)
        if k < SEQ_DEV - 1:
            decay = got_ref[j, DK:STATE_ROWS, :][0:1].astype(f32)
            carried = carried * decay + got_ref[j, 0:DK, :].astype(f32)


def attend_kernel(
    tp_ref, query_ref, mine_ref, other_ref, up_ref, cos_ref, sin_ref, out_ref, lw_ref, ex_ref, rope_ref
):
    up = up_ref[:, pl.ds(pl.multiple_of(tp_ref[0] * HEADS * 128, HEADS * 128), HEADS * 128)]
    lane32 = iota2((32, 128), 1)
    in_rope = (lane32 >= NOPE) & (lane32 < NOPE + ROPE)
    for c in range(2):
        for j in range(SEQ_DEV):
            ref, base = (mine_ref, STATE_ROWS) if c == 0 else (other_ref, 0)
            lat = jnp.concatenate(
                [ref[j, base : base + 128, :], ref[j, base + 128 : base + 256, :]], axis=1
            )
            at = (c * SEQ_DEV + j) * 128
            ex_ref[at : at + 128, :] = dot(lat, up).astype(bf16)
            packed = ref[j, base + 256 : base + 288, :].astype(f32)
            for g in range(4):
                piece = pltpu.roll(packed, (NOPE - 32 * g) % 128, 1)
                rope_ref[at + 32 * g : at + 32 * g + 32, :] = jnp.where(in_rope, piece, 0.0).astype(bf16)
    lane = iota2((TOK, 128), 1)
    q_blocks = [query_ref[:, 128 * i : 128 * i + 128].astype(f32) for i in range(3)]
    key_lane = iota2((SEQ_DEV * TOK, 128), 1)
    for h in range(HEADS):
        lanes = slice(h * 128, (h + 1) * 128)
        if h == 0:
            q = q_blocks[0]
        elif h == 1:
            q = jnp.where(lane < 32, pltpu.roll(q_blocks[0], 32, 1), pltpu.roll(q_blocks[1], 32, 1))
        elif h == 2:
            q = jnp.where(lane < 64, pltpu.roll(q_blocks[1], 64, 1), pltpu.roll(q_blocks[2], 64, 1))
        else:
            q = pltpu.roll(q_blocks[2], 96, 1)
        q = rotated(q, cos_ref[...], sin_ref[...]).astype(bf16)
        ex = ex_ref[:, lanes]
        keys = jnp.where(key_lane < NOPE, ex, rope_ref[...])
        scores = dot(q, keys, NT)
        peak = jnp.max(scores, axis=1, keepdims=True)
        weights = jnp.exp2((scores - peak) * (SCALE * LOG2E))
        total = jnp.sum(weights, axis=1, keepdims=True)
        mixed = dot(weights.astype(bf16), ex) / total
        lw_ref[:, h : h + 1] = peak * SCALE + jnp.log(total)
        if h % 2 == 0:
            kept = pltpu.roll(mixed, 64, 1)
        else:
            out_ref[:, (h // 2) * 128 : (h // 2) * 128 + 128] = jnp.where(
                lane < 64, kept, mixed
            ).astype(bf16)


def finish_kernel(
    idx_ref, local_ref, damped_ref, state_ref, gain_ref, att_ref,
    own_ref, left_ref, right_ref, far_a_ref, far_b_ref, send_ref, keep_ref, act_ref,
):
    tp = idx_ref[0]
    for part in range(2):
        start = jnp.where(tp == part, HALF, 0)
        at = pl.ds(pl.multiple_of(start, HALF), HALF)
        to = slice(part * HALF, (part + 1) * HALF)
        for h in range(HEADS):
            lanes = slice(h * DK, (h + 1) * DK)
            o = (
                local_ref[at, lanes]
                + dot(damped_ref[0, at, lanes], state_ref[h], NT)
                + dot(damped_ref[1, at, lanes], state_ref[HEADS + h], NT)
            )
            mean = jnp.sum(o * o, axis=1, keepdims=True) * (1.0 / DK)
            act_ref[to, lanes] = (o * lax.rsqrt(mean + EPS) * gain_ref[:, lanes]).astype(bf16)
        act_ref[to, HEADS * DK :] = att_ref[at, :]
    act = act_ref[...]
    for i in range(4):
        if i < 3:
            got = dot(act, (own_ref, left_ref, right_ref)[i][...])
        else:
            got = dot(act[:, :384], far_a_ref[...]) + dot(act[:, 384:], far_b_ref[...])
        got = got.astype(bf16)
        lanes = pl.ds(pl.multiple_of(idx_ref[1 + i] * 512, 512), 512)
        send_ref[:, lanes] = got[:HALF]
        keep_ref[:, lanes] = got[HALF:]


def call(kernel, outs, *args, scratch=(), flops=0, name=None, smem=0):
    specs = [
        pl.BlockSpec(memory_space=pltpu.SMEM) if i < smem else pl.BlockSpec(memory_space=pltpu.VMEM)
        for i in range(len(args))
    ]
    single = not isinstance(outs, tuple)
    return pl.pallas_call(
        kernel,
        out_shape=outs,
        in_specs=specs,
        out_specs=pl.BlockSpec(memory_space=pltpu.VMEM)
        if single
        else tuple(pl.BlockSpec(memory_space=pltpu.VMEM) for _ in outs),
        scratch_shapes=list(scratch),
        cost_estimate=pl.CostEstimate(flops=flops, bytes_accessed=1 << 20, transcendentals=0),
        name=name,
    )(*args)


def shape(dims, dtype):
    return jax.ShapeDtypeStruct(dims, dtype)


def ring(n, step):
    return [(i, (i + step) % n) for i in range(n)]


def exchange(value):
    return lax.all_to_all(value, "sp_1", split_axis=0, concat_axis=0, tiled=True)


def local(
    recurrent_query,
    forget_logits,
    recurrent_value,
    forget_floor,
    extra_log_decay,
    recurrent_norm_gain,
    attention_query,
    latent,
    rotary_key,
    latent_norm_gain,
    latent_up_weight,
    recurrent_output_weight,
    attention_output_weight,
):
    place = lax.axis_index("sp_1")
    column = lax.axis_index("fs")
    tp = lax.axis_index("tp")
    lane = np.arange(128)
    inverse = np.power(
        np.float32(ROPE_BASE), (-(lane % 16).astype(np.float32) / np.float32(16)), dtype=np.float32
    )
    position = (place * TOK + jnp.arange(TOK)).astype(f32)
    angle = position[:, None] * inverse[None, :]
    first = (lane >= NOPE) & (lane < NOPE + ROPE // 2)
    second = (lane >= NOPE + ROPE // 2) & (lane < NOPE + ROPE)
    cos_table = jnp.where(first | second, jnp.cos(angle), (lane < NOPE).astype(np.float32))
    sin_table = jnp.sin(angle) * (second.astype(np.float32) - first.astype(np.float32))

    tp_at = tp.astype(jnp.int32).reshape(1)
    logits, values, extra = forget_logits[0], recurrent_value[0], extra_log_decay[0]
    padded_key = jnp.pad(rotary_key[0], ((0, 0), (NOPE, 128 - NOPE - ROPE)))

    sent = call(
        send_kernel,
        shape((SEQ_DEV, CHUNK_ROWS, DK), bf16),
        tp_at, logits, values, forget_floor, extra, latent[0], latent_norm_gain.reshape(1, RANK),
        padded_key, cos_table, sin_table,
        flops=1 << 29, name="send", smem=1,
    )
    got = exchange(sent)

    weights = jnp.concatenate([recurrent_output_weight, attention_output_weight], axis=0)
    from_left = lax.ppermute(weights, "fs", ring(4, 1))
    from_right = lax.ppermute(weights, "fs", ring(4, -1))
    far_a = lax.ppermute(from_left[:384], "fs", ring(4, 1))
    far_b = lax.ppermute(from_right[384:], "fs", ring(4, -1))

    local_out, damped = call(
        local_kernel,
        (shape((TOK, HEADS * DK), f32), shape((2, TOK, HEADS * DK), bf16)),
        recurrent_query[0], logits, values, forget_floor, extra,
        flops=1 << 30, name="local",
    )

    scanned = call(
        scan_kernel,
        shape((SEQ_DEV, DK, DK), bf16),
        (place // HEADS).astype(jnp.int32).reshape(1), got,
        flops=1 << 26, name="scan", smem=1,
    )
    states = exchange(scanned)

    other = lax.ppermute(got[:, STATE_ROWS:], "tp", [(0, 1), (1, 0)])
    attended, log_weight = call(
        attend_kernel,
        (shape((TOK, HEADS * 64), bf16), shape((TOK, HEADS), f32)),
        tp_at, attention_query[0], got, other, latent_up_weight, cos_table, sin_table,
        scratch=(pltpu.VMEM((SEQ_DEV * TOK, HEADS * 128), bf16), pltpu.VMEM((SEQ_DEV * TOK, 128), bf16)),
        flops=1 << 31, name="attend", smem=1,
    )

    index = jnp.stack([tp, column, (column + 3) % 4, (column + 1) % 4, (column + 2) % 4]).astype(jnp.int32)
    send, keep = call(
        finish_kernel,
        (shape((HALF, 2048), bf16), shape((HALF, 2048), bf16)),
        index, local_out, damped, states, recurrent_norm_gain.reshape(1, HEADS * DK), attended,
        weights, from_left, from_right, far_a, far_b,
        scratch=(pltpu.VMEM((TOK, 768), bf16),),
        flops=1 << 30, name="finish", smem=1,
    )
    arrived = lax.ppermute(send, "tp", [(0, 1), (1, 0)])
    mixed = (keep.astype(f32) + arrived.astype(f32)).astype(bf16)
    return mixed[None], log_weight[None]


def solution(mesh):
    torus = Mesh(
        mesh.devices.reshape(8, 8, mesh.shape["fs"], mesh.shape["tp"]), ("sp_0", "sp_1", "fs", "tp")
    )
    in_specs = (
        P("fs", SP, "tp"),
        P("fs", SP, "tp"),
        P("fs", SP, "tp"),
        P(None, "tp"),
        P("fs", SP, "tp"),
        P("tp"),
        P("fs", SP, "tp"),
        P("fs", SP, None),
        P("fs", SP, None),
        P(),
        P(),
        P("tp", "fs"),
        P("tp", "fs"),
    )
    out_specs = (P("fs", SP_TP, None), P("fs", SP, "tp"))
    return jax.shard_map(local, mesh=torus, in_specs=in_specs, out_specs=out_specs, check_vma=False)
```

```python
import numpy as np

import jax
import jax.numpy as jnp
from jax import lax
from jax.experimental import pallas as pl
from jax.experimental.pallas import tpu as pltpu
from jax.sharding import Mesh
from jax.sharding import PartitionSpec as P


DK = 128
HEADS = 4
NOPE = 64
ROPE = 32
RANK = 256
BLOCK = 64
TOK = 256
HALF = 128
SEQ_DEV = 8
STATE_ROWS = 144
KV_ROWS = 288
CHUNK_ROWS = STATE_ROWS + KV_ROWS
SP = ("sp_0", "sp_1")
SP_TP = ("sp_0", "sp_1", "tp")
EPS = 1e-06
ROPE_BASE = 10000.0
SCALE = (NOPE + ROPE) ** (-0.5)
LOG2E = 1.4426950408889634

f32 = jnp.float32
bf16 = jnp.bfloat16
NT = (((1,), (1,)), ((), ()))
TN = (((0,), (0,)), ((), ()))


def dot(a, b, dims=(((1,), (0,)), ((), ()))):
    return lax.dot_general(a, b, dims, preferred_element_type=f32)


def iota2(shape, axis):
    return lax.broadcasted_iota(jnp.int32, shape, axis)


def exact_sum(selector, values):
    high = values.astype(bf16)
    low = (values - high.astype(f32)).astype(bf16)
    return dot(selector, high) + dot(selector, low)


def start_all(sems, pairs):
    copies = [pltpu.make_async_copy(src, dst, sems.at[i]) for i, (src, dst) in enumerate(pairs)]
    for copy in copies:
        copy.start()
    return copies


def shut(logit):
    return 0.5 - 0.5 * jnp.tanh(0.5 * logit)


def gate(closed, floor, extra):
    keyed = (1.0 - floor) * closed
    return keyed, jnp.log(1.0 - keyed) + extra


def head_extra(extra_ref, first, count):
    return jnp.concatenate(
        [
            jnp.transpose(jnp.broadcast_to(extra_ref[h : h + 1, :], (DK, TOK)))
            for h in range(first, first + count)
        ],
        axis=1,
    )


def rotated(x, cos_table, sin_table):
    lane = iota2(x.shape, 1)
    partner = jnp.where(lane < NOPE + ROPE // 2, pltpu.roll(x, 128 - 16, 1), pltpu.roll(x, 16, 1))
    return x * cos_table + partner * sin_table


def send_kernel(
    logit_hbm, value_hbm, floor_hbm, extra_hbm, lat_hbm, gain_hbm, key_hbm, cos_hbm, sin_hbm,
    upper_hbm, lower_hbm,
    out_hbm, weight_hbm,
    logit_ref, value_ref, floor_ref, extra_ref, lat_ref, gain_ref, key_ref, cos_ref, sin_ref,
    state_ref, kv_ref, weight_ref, in_sems, kv_sems, state_sems, weight_sem,
):
    tp, place = lax.axis_index("tp"), lax.axis_index("sp_1")
    mine = pl.ds(pl.multiple_of(tp * HALF, HALF), HALF)
    spot = pl.ds(pl.multiple_of(place * TOK + tp * HALF, HALF), HALF)
    loads = start_all(
        in_sems,
        [
            (lat_hbm.at[mine, :], lat_ref),
            (gain_hbm, gain_ref),
            (key_hbm, key_ref),
            (cos_hbm.at[:, spot], cos_ref),
            (sin_hbm.at[:, spot], sin_ref),
            (logit_hbm, logit_ref),
            (extra_hbm, extra_ref),
            (floor_hbm, floor_ref),
            (value_hbm, value_ref),
            (upper_hbm, weight_ref.at[0:512, :]),
            (lower_hbm, weight_ref.at[512:768, :]),
        ],
    )
    for load in loads[:5]:
        load.wait()
    wide = lat_ref[...].astype(f32)
    mean = jnp.sum(wide * wide, axis=1, keepdims=True) * (1.0 / RANK)
    normed = (wide * lax.rsqrt(mean + EPS) * gain_ref[...]).astype(bf16)
    key = key_ref[:, mine].astype(f32)
    cos, sin = cos_ref[...], sin_ref[...]
    turned = jnp.concatenate(
        [key[:16] * cos - key[16:] * sin, key[:16] * sin + key[16:] * cos], axis=0
    ).astype(bf16)
    kv_ref[0:128, :] = normed[:, :128]
    kv_ref[128:256, :] = normed[:, 128:]
    kv_ref[256:KV_ROWS, :] = turned
    stores = start_all(
        kv_sems,
        [(kv_ref, out_hbm.at[q, STATE_ROWS:CHUNK_ROWS, :]) for q in range(SEQ_DEV)],
    )
    for load in loads[5:9]:
        load.wait()
    rows = iota2((TOK, TOK), 0)
    cols = iota2((TOK, TOK), 1)
    after = (cols > rows).astype(f32).astype(bf16)
    before = (cols < rows).astype(f32).astype(bf16)
    for pair in range(HEADS // 2):
        if pair == 1:
            for load in loads[9:]:
                load.wait()
            weight_store = pltpu.make_async_copy(weight_ref, weight_hbm, weight_sem)
            weight_store.start()
            stores.append(weight_store)
        lanes = slice(pair * 2 * DK, (pair + 1) * 2 * DK)
        closed = shut(logit_ref[:, lanes].astype(f32))
        extra = head_extra(extra_ref, 2 * pair, 2)
        for d in range(2):
            keyed, decay = gate(closed, floor_ref[d : d + 1, lanes], extra)
            left = exact_sum(after if d == 0 else before, decay)
            edge = 0 if d == 0 else TOK - 1
            total = jnp.exp(left[edge : edge + 1] + decay[edge : edge + 1])
            weighted = (keyed * jnp.exp(left)).astype(bf16)
            for s in range(2):
                h = 2 * pair + s
                at = d * HEADS + h
                state = dot(
                    value_ref[:, h * DK : (h + 1) * DK], weighted[:, s * DK : (s + 1) * DK], TN
                )
                state_ref[at, 0:DK, :] = state.astype(bf16)
                state_ref[at, DK:STATE_ROWS, :] = jnp.broadcast_to(
                    total[:, s * DK : (s + 1) * DK], (STATE_ROWS - DK, DK)
                ).astype(bf16)
                store = pltpu.make_async_copy(
                    state_ref.at[at], out_hbm.at[at, 0:STATE_ROWS, :], state_sems.at[at]
                )
                store.start()
                stores.append(store)
    for store in stores:
        store.wait()


def local_kernel(
    query_ref, logit_ref, value_ref, floor_ref, extra_ref, out_hbm, damped_hbm, out_ref, damped_ref, sems
):
    stores = []
    rows = iota2((TOK, TOK), 0)
    cols = iota2((TOK, TOK), 1)
    same = (rows // BLOCK) == (cols // BLOCK)
    lower = same & (cols <= rows)
    upper = same & (cols >= rows)
    blocks = TOK // BLOCK
    for h in range(HEADS):
        lanes = slice(h * DK, (h + 1) * DK)
        closed = shut(logit_ref[:, lanes].astype(f32))
        extra = head_extra(extra_ref, h, 1)
        query = query_ref[:, lanes].astype(f32)
        value = value_ref[:, lanes]
        outs = [None] * blocks
        inner_sum = jnp.zeros((TOK, DK), f32)
        for d in range(2):
            seen = lower if d == 0 else upper
            keyed, decay = gate(closed, floor_ref[d : d + 1, lanes], extra)
            within = exact_sum(seen.astype(f32).astype(bf16), decay)
            damped = query * jnp.exp(within)
            grown = (keyed * jnp.exp(-within)).astype(bf16)
            damped16 = damped.astype(bf16)
            scores = jnp.where(seen, dot(damped16, grown, NT), 0.0).astype(bf16)
            inner_sum = inner_sum + dot(scores, value)
            state = None
            offset = jnp.zeros((1, DK), f32)
            for b in range(blocks) if d == 0 else reversed(range(blocks)):
                at = slice(b * BLOCK, (b + 1) * BLOCK)
                edge = (b + 1) * BLOCK - 1 if d == 0 else b * BLOCK
                total = within[edge : edge + 1]
                damped_ref[d, at, lanes] = (damped[at] * jnp.exp(offset)).astype(bf16)
                if state is not None:
                    cross = dot(damped16[at], state.astype(bf16), NT)
                    outs[b] = cross if outs[b] is None else outs[b] + cross
                offset = offset + total
                if b == (blocks - 1 if d == 0 else 0):
                    continue
                weighted = (keyed[at] * jnp.exp(total - within[at])).astype(bf16)
                added = dot(value[at], weighted, TN)
                state = added if state is None else state * jnp.exp(total) + added
        for b in range(blocks):
            at = slice(b * BLOCK, (b + 1) * BLOCK)
            out_ref[at, lanes] = inner_sum[at] if outs[b] is None else inner_sum[at] + outs[b]
        stores.append(pltpu.make_async_copy(out_ref.at[:, lanes], out_hbm.at[:, lanes], sems.at[h, 0]))
        stores.append(
            pltpu.make_async_copy(damped_ref.at[:, :, lanes], damped_hbm.at[:, :, lanes], sems.at[h, 1])
        )
        for store in stores[-2:]:
            store.start()
    for store in stores:
        store.wait()


def scan_kernel(got_ref, out_ref):
    d = lax.axis_index("sp_1") // HEADS
    carried = jnp.zeros((DK, DK), f32)
    for k in range(SEQ_DEV):
        j = jnp.where(d == 0, k, SEQ_DEV - 1 - k)
        out_ref[j] = carried.astype(bf16)
        if k < SEQ_DEV - 1:
            decay = got_ref[j, DK:STATE_ROWS, :][0:1].astype(f32)
            carried = carried * decay + got_ref[j, 0:DK, :].astype(f32)


def unpack_rope(rope_ref, ref, base):
    for j in range(SEQ_DEV):
        turned = ref[j, base + 256 : base + 288, :].astype(f32)
        rope_ref[j * 128 : j * 128 + 128, :] = jnp.transpose(
            jnp.concatenate([jnp.zeros((NOPE, 128), f32), turned, jnp.zeros((32, 128), f32)], axis=0)
        ).astype(bf16)


def expand(ex_ref, ref, base, up_ref):
    up = up_ref[:, pl.ds(pl.multiple_of(lax.axis_index("tp") * HEADS * 128, HEADS * 128), HEADS * 128)]
    for j in range(SEQ_DEV):
        lat = jnp.concatenate(
            [ref[j, base : base + 128, :], ref[j, base + 128 : base + 256, :]], axis=1
        )
        ex_ref[j * 128 : j * 128 + 128, :] = dot(lat, up).astype(bf16)


def expand_kernel(got_ref, up_ref, ex_ref, rope_ref):
    unpack_rope(rope_ref, got_ref, STATE_ROWS)
    expand(ex_ref, got_ref, STATE_ROWS, up_ref)


def attend_kernel(
    query_ref, other_ref, ex_mine_ref, rope_mine_ref, up_ref, cos_ref, sin_ref, local_hbm, damped_hbm,
    gain_hbm,
    out_ref, lw_ref, local_ref, damped_ref, gain_ref,
    ex_ref, rope_ref, sems,
):
    loads = start_all(
        sems, [(local_hbm, local_ref), (damped_hbm, damped_ref), (gain_hbm, gain_ref)]
    )
    unpack_rope(rope_ref, other_ref, 0)
    expand(ex_ref, other_ref, 0, up_ref)
    spot = pl.ds(pl.multiple_of(lax.axis_index("sp_1") * TOK, TOK), TOK)
    cos, sin = cos_ref[:, spot], sin_ref[:, spot]
    nothing = jnp.zeros((NOPE, TOK), f32)
    cos_table = jnp.transpose(jnp.concatenate([nothing + 1.0, cos, cos, nothing[:32]], axis=0))
    sin_table = jnp.transpose(jnp.concatenate([nothing, -sin, sin, nothing[:32]], axis=0))
    log_weights = []
    lane = iota2((TOK, 128), 1)
    q_blocks = [query_ref[:, 128 * i : 128 * i + 128].astype(f32) for i in range(3)]
    key_lane = iota2((SEQ_DEV * HALF, 128), 1)
    for h in range(HEADS):
        lanes = slice(h * 128, (h + 1) * 128)
        if h == 0:
            q = q_blocks[0]
        elif h == 1:
            q = jnp.where(lane < 32, pltpu.roll(q_blocks[0], 32, 1), pltpu.roll(q_blocks[1], 32, 1))
        elif h == 2:
            q = jnp.where(lane < 64, pltpu.roll(q_blocks[1], 64, 1), pltpu.roll(q_blocks[2], 64, 1))
        else:
            q = pltpu.roll(q_blocks[2], 96, 1)
        q = rotated(q, cos_table, sin_table).astype(bf16)
        parts = []
        for ex_part, rope_part in ((ex_mine_ref, rope_mine_ref), (ex_ref, rope_ref)):
            ex = ex_part[:, lanes]
            parts.append((ex, dot(q, jnp.where(key_lane < NOPE, ex, rope_part[...]), NT)))
        peak = jnp.maximum(
            jnp.max(parts[0][1], axis=1, keepdims=True), jnp.max(parts[1][1], axis=1, keepdims=True)
        )
        total, mixed = 0.0, 0.0
        for ex, scores in parts:
            weights = jnp.exp2((scores - peak) * (SCALE * LOG2E))
            total = total + jnp.sum(weights, axis=1, keepdims=True)
            mixed = mixed + dot(weights.astype(bf16), ex)
        mixed = mixed / total
        log_weights.append(jnp.broadcast_to(peak * SCALE + jnp.log(total), (TOK, 32)))
        if h % 2 == 0:
            kept = pltpu.roll(mixed, 64, 1)
        else:
            out_ref[:, (h // 2) * 128 : (h // 2) * 128 + 128] = jnp.where(
                lane < 64, kept, mixed
            ).astype(bf16)
    turned = jnp.transpose(jnp.concatenate(log_weights, axis=1))
    for h in range(HEADS):
        lw_ref[h : h + 1, :] = turned[32 * h : 32 * h + 1]
    for load in loads:
        load.wait()


def finish_kernel(
    local_ref, damped_ref, state_ref, gain_ref, att_ref, own_hbm, left_hbm, right_hbm, far_hbm,
    send_ref, keep_ref,
    weight_ref, act_ref, sems,
):
    tp, column = lax.axis_index("tp"), lax.axis_index("fs")
    loads = start_all(
        sems,
        [(ref, weight_ref.at[i]) for i, ref in enumerate((own_hbm, left_hbm, right_hbm, far_hbm))],
    )
    for part in range(2):
        start = jnp.where(tp == part, HALF, 0)
        at = pl.ds(pl.multiple_of(start, HALF), HALF)
        to = slice(part * HALF, (part + 1) * HALF)
        for h in range(HEADS):
            lanes = slice(h * DK, (h + 1) * DK)
            o = (
                local_ref[at, lanes]
                + dot(damped_ref[0, at, lanes], state_ref[h], NT)
                + dot(damped_ref[1, at, lanes], state_ref[HEADS + h], NT)
            )
            mean = jnp.sum(o * o, axis=1, keepdims=True) * (1.0 / DK)
            act_ref[to, lanes] = (o * lax.rsqrt(mean + EPS) * gain_ref[:, lanes]).astype(bf16)
        act_ref[to, HEADS * DK :] = att_ref[at, :]
    act = act_ref[...]
    for i in range(4):
        loads[i].wait()
        got = dot(act, weight_ref[i]).astype(bf16)
        lanes = pl.ds(pl.multiple_of(((column + (0, 3, 1, 2)[i]) % 4) * 512, 512), 512)
        send_ref[:, lanes] = got[:HALF]
        keep_ref[:, lanes] = got[HALF:]


SPACES = {"v": pltpu.VMEM, "h": pltpu.HBM}


def call(kernel, ins, outs, *args, scratch=(), flops=0, mib=16):
    args = [
        pltpu.with_memory_space_constraint(a, pltpu.HBM) if c == "h" else a for c, a in zip(ins, args)
    ]
    many = isinstance(outs, tuple)
    spaces = [
        pltpu.HBM if isinstance(o, HbmOut) else pltpu.VMEM for o in (outs if many else (outs,))
    ]
    shapes = tuple(
        pltpu.HBM(o.dims, o.dtype) if isinstance(o, HbmOut) else o for o in (outs if many else (outs,))
    )
    specs = tuple(pl.BlockSpec(memory_space=space) for space in spaces)
    return pl.pallas_call(
        kernel,
        out_shape=shapes if many else shapes[0],
        in_specs=[pl.BlockSpec(memory_space=SPACES[c]) for c in ins],
        out_specs=specs if many else specs[0],
        scratch_shapes=list(scratch),
        cost_estimate=pl.CostEstimate(flops=flops, bytes_accessed=1 << 20, transcendentals=0),
        compiler_params=pltpu.CompilerParams(vmem_limit_bytes=mib << 20),
    )(*args)


class HbmOut:
    def __init__(self, dims, dtype):
        self.dims, self.dtype = dims, dtype


def shape(dims, dtype):
    return jax.ShapeDtypeStruct(dims, dtype)


def ring(n, step):
    return [(i, (i + step) % n) for i in range(n)]


def exchange(value):
    return lax.all_to_all(value, "sp_1", split_axis=0, concat_axis=0, tiled=True)


def local(
    recurrent_query,
    forget_logits,
    recurrent_value,
    forget_floor,
    extra_log_decay,
    recurrent_norm_gain,
    attention_query,
    latent,
    rotary_key,
    latent_norm_gain,
    latent_up_weight,
    recurrent_output_weight,
    attention_output_weight,
):
    cos_table, sin_table = rotary_tables()
    logits, values = forget_logits[0], recurrent_value[0]
    extra = jnp.swapaxes(extra_log_decay[0], 0, 1)

    sent, weights = call(
        send_kernel,
        "h" * 11,
        (HbmOut((SEQ_DEV, CHUNK_ROWS, DK), bf16), HbmOut((768, 512), bf16)),
        logits, values, forget_floor, extra, latent[0], latent_norm_gain.reshape(1, RANK),
        jnp.swapaxes(rotary_key[0], 0, 1), cos_table, sin_table,
        recurrent_output_weight, attention_output_weight,
        scratch=(
            pltpu.VMEM((TOK, HEADS * DK), bf16),
            pltpu.VMEM((TOK, HEADS * DK), bf16),
            pltpu.VMEM((2, HEADS * DK), f32),
            pltpu.VMEM((HEADS, TOK), f32),
            pltpu.VMEM((HALF, RANK), bf16),
            pltpu.VMEM((1, RANK), f32),
            pltpu.VMEM((ROPE, TOK), bf16),
            pltpu.VMEM((16, HALF), f32),
            pltpu.VMEM((16, HALF), f32),
            pltpu.VMEM((2 * HEADS, STATE_ROWS, DK), bf16),
            pltpu.VMEM((KV_ROWS, DK), bf16),
            pltpu.VMEM((768, 512), bf16),
            pltpu.SemaphoreType.DMA((11,)),
            pltpu.SemaphoreType.DMA((SEQ_DEV,)),
            pltpu.SemaphoreType.DMA((2 * HEADS,)),
            pltpu.SemaphoreType.DMA,
        ),
        flops=1 << 29, mib=14,
    )
    got = exchange(sent)

    from_left = lax.ppermute(weights, "fs", ring(4, 1))
    from_right = lax.ppermute(weights, "fs", ring(4, -1))
    far = lax.ppermute(weights, "fs", ring(4, 2))

    local_out, damped = call(
        local_kernel,
        "vvvvv",
        (HbmOut((TOK, HEADS * DK), f32), HbmOut((2, TOK, HEADS * DK), bf16)),
        recurrent_query[0], logits, values, forget_floor, extra,
        scratch=(
            pltpu.VMEM((TOK, HEADS * DK), f32),
            pltpu.VMEM((2, TOK, HEADS * DK), bf16),
            pltpu.SemaphoreType.DMA((HEADS, 2)),
        ),
        flops=1 << 30, mib=14,
    )

    scanned = call(
        scan_kernel, "v", shape((SEQ_DEV, DK, DK), bf16), got,
        flops=1 << 26, mib=8,
    )
    states = exchange(scanned)

    other = lax.ppermute(got[:, STATE_ROWS:], "tp", [(0, 1), (1, 0)])
    keys = SEQ_DEV * HALF
    ex_mine, rope_mine = call(
        expand_kernel, "vv",
        (shape((keys, HEADS * 128), bf16), shape((keys, 128), bf16)),
        got, latent_up_weight,
        flops=1 << 28, mib=12,
    )
    attended, log_weight, local_out, damped, gain = call(
        attend_kernel,
        "v" * 7 + "hhh",
        (
            shape((TOK, HEADS * 64), bf16),
            shape((HEADS, TOK), f32),
            shape((TOK, HEADS * DK), f32),
            shape((2, TOK, HEADS * DK), bf16),
            shape((1, HEADS * DK), f32),
        ),
        attention_query[0], other, ex_mine, rope_mine, latent_up_weight, cos_table, sin_table,
        local_out, damped, recurrent_norm_gain.reshape(1, HEADS * DK),
        scratch=(
            pltpu.VMEM((keys, HEADS * 128), bf16),
            pltpu.VMEM((keys, 128), bf16),
            pltpu.SemaphoreType.DMA((3,)),
        ),
        flops=1 << 31, mib=24,
    )

    send, keep = call(
        finish_kernel,
        "v" * 5 + "h" * 4,
        (shape((HALF, 2048), bf16), shape((HALF, 2048), bf16)),
        local_out, damped, states, gain, attended, weights, from_left, from_right, far,
        scratch=(
            pltpu.VMEM((4, 768, 512), bf16),
            pltpu.VMEM((TOK, 768), bf16),
            pltpu.SemaphoreType.DMA((4,)),
        ),
        flops=1 << 30, mib=16,
    )
    arrived = lax.ppermute(send, "tp", [(0, 1), (1, 0)])
    mixed = (keep.astype(f32) + arrived.astype(f32)).astype(bf16)
    return mixed[None], jnp.swapaxes(log_weight, 0, 1)[None]


def rotary_tables():
    inverse = np.power(
        np.float32(ROPE_BASE), -np.arange(16, dtype=np.float32) / np.float32(16), dtype=np.float32
    )
    angle = inverse[:, None] * np.arange(SEQ_DEV * TOK, dtype=np.float32)[None, :]
    angle = angle.astype(np.float64)
    return np.cos(angle).astype(np.float32), np.sin(angle).astype(np.float32)


def solution(mesh):
    torus = Mesh(
        mesh.devices.reshape(8, 8, mesh.shape["fs"], mesh.shape["tp"]), ("sp_0", "sp_1", "fs", "tp")
    )
    in_specs = (
        P("fs", SP, "tp"),
        P("fs", SP, "tp"),
        P("fs", SP, "tp"),
        P(None, "tp"),
        P("fs", SP, "tp"),
        P("tp"),
        P("fs", SP, "tp"),
        P("fs", SP, None),
        P("fs", SP, None),
        P(),
        P(),
        P("tp", "fs"),
        P("tp", "fs"),
    )
    out_specs = (P("fs", SP_TP, None), P("fs", SP, "tp"))
    return jax.shard_map(local, mesh=torus, in_specs=in_specs, out_specs=out_specs, check_vma=False)
```

```python
import numpy as np

import jax
import jax.numpy as jnp
from jax import lax
from jax.experimental import pallas as pl
from jax.experimental.pallas import tpu as pltpu
from jax.sharding import Mesh
from jax.sharding import PartitionSpec as P


DK = 128
HEADS = 4
NOPE = 64
ROPE = 32
RANK = 256
BLOCK = 64
TOK = 256
HALF = 128
SEQ_DEV = 8
STATE_ROWS = 136
KV_ROWS = 144
CHUNK_ROWS = STATE_ROWS + KV_ROWS
SP = ("sp_0", "sp_1")
SP_TP = ("sp_0", "sp_1", "tp")
EPS = 1e-06
ROPE_BASE = 10000.0
SCALE = (NOPE + ROPE) ** (-0.5)
LOG2E = 1.4426950408889634

f32 = jnp.float32
bf16 = jnp.bfloat16
NT = (((1,), (1,)), ((), ()))
TN = (((0,), (0,)), ((), ()))


def dot(a, b, dims=(((1,), (0,)), ((), ()))):
    return lax.dot_general(a, b, dims, preferred_element_type=f32)


def iota2(shape, axis):
    return lax.broadcasted_iota(jnp.int32, shape, axis)


def exact_sum(selector, values):
    high = values.astype(bf16)
    low = (values - high.astype(f32)).astype(bf16)
    return dot(selector, high) + dot(selector, low)


def start_all(sems, pairs):
    copies = [pltpu.make_async_copy(src, dst, sems.at[i]) for i, (src, dst) in enumerate(pairs)]
    for copy in copies:
        copy.start()
    return copies


def shut(logit):
    return 0.5 - 0.5 * jnp.tanh(0.5 * logit)


def gate(closed, floor, extra):
    keyed = (1.0 - floor) * closed
    return keyed, jnp.log(1.0 - keyed) + extra


def head_extra(extra_ref, first, count):
    return jnp.concatenate(
        [
            jnp.transpose(jnp.broadcast_to(extra_ref[h : h + 1, :], (DK, TOK)))
            for h in range(first, first + count)
        ],
        axis=1,
    )


def rotated(x, cos_table, sin_table):
    lane = iota2(x.shape, 1)
    partner = jnp.where(lane < NOPE + ROPE // 2, pltpu.roll(x, 128 - 16, 1), pltpu.roll(x, 16, 1))
    return x * cos_table + partner * sin_table


def send_kernel(
    logit_hbm, value_hbm, floor_hbm, extra_hbm, lat_hbm, gain_hbm, key_hbm, cos_hbm, sin_hbm,
    out_hbm,
    logit_ref, value_ref, floor_ref, extra_ref, lat_ref, gain_ref, key_ref, cos_ref, sin_ref,
    state_ref, kv_ref, in_sems, kv_sems, state_sems,
):
    tp, place = lax.axis_index("tp"), lax.axis_index("sp_1")
    mine = pl.ds(pl.multiple_of(tp * HALF, HALF), HALF)
    spot = pl.ds(pl.multiple_of(place * TOK + tp * HALF, HALF), HALF)
    loads = start_all(
        in_sems,
        [
            (lat_hbm.at[mine, :], lat_ref),
            (gain_hbm, gain_ref),
            (key_hbm, key_ref),
            (cos_hbm.at[:, spot], cos_ref),
            (sin_hbm.at[:, spot], sin_ref),
            (logit_hbm, logit_ref),
            (extra_hbm, extra_ref),
            (floor_hbm, floor_ref),
            (value_hbm, value_ref),
        ],
    )
    for load in loads[:5]:
        load.wait()
    wide = lat_ref[...].astype(f32)
    mean = jnp.sum(wide * wide, axis=1, keepdims=True) * (1.0 / RANK)
    normed = (wide * lax.rsqrt(mean + EPS) * gain_ref[...]).astype(bf16)
    key = key_ref[:, mine].astype(f32)
    cos, sin = cos_ref[...], sin_ref[...]
    turned = jnp.concatenate(
        [key[:16] * cos - key[16:] * sin, key[:16] * sin + key[16:] * cos], axis=0
    )
    for p in range(2):
        kv_ref[p, 0:128, :] = normed[:, p * 128 : (p + 1) * 128]
        kv_ref[p, 128:KV_ROWS, :] = turned[p * 16 : (p + 1) * 16].astype(bf16)
    stores = start_all(
        kv_sems,
        [(kv_ref.at[q % 2], out_hbm.at[q, STATE_ROWS:CHUNK_ROWS, :]) for q in range(SEQ_DEV)],
    )
    for load in loads[5:]:
        load.wait()
    rows = iota2((TOK, TOK), 0)
    cols = iota2((TOK, TOK), 1)
    after = (cols > rows).astype(f32).astype(bf16)
    before = (cols < rows).astype(f32).astype(bf16)
    for pair in range(HEADS // 2):
        lanes = slice(pair * 2 * DK, (pair + 1) * 2 * DK)
        closed = shut(logit_ref[:, lanes].astype(f32))
        extra = head_extra(extra_ref, 2 * pair, 2)
        for d in range(2):
            keyed, decay = gate(closed, floor_ref[d : d + 1, lanes], extra)
            left = exact_sum(after if d == 0 else before, decay)
            edge = 0 if d == 0 else TOK - 1
            total = jnp.exp(left[edge : edge + 1] + decay[edge : edge + 1])
            weighted = (keyed * jnp.exp(left)).astype(bf16)
            for s in range(2):
                h = 2 * pair + s
                at = d * HEADS + h
                state = dot(
                    value_ref[:, h * DK : (h + 1) * DK], weighted[:, s * DK : (s + 1) * DK], TN
                )
                state_ref[at, 0:DK, :] = state.astype(bf16)
                state_ref[at, DK:STATE_ROWS, :] = jnp.broadcast_to(
                    total[:, s * DK : (s + 1) * DK], (STATE_ROWS - DK, DK)
                ).astype(bf16)
                store = pltpu.make_async_copy(
                    state_ref.at[at], out_hbm.at[at, 0:STATE_ROWS, :], state_sems.at[at]
                )
                store.start()
                stores.append(store)
    for store in stores:
        store.wait()


def local_kernel(
    query_ref, logit_ref, value_ref, floor_ref, extra_ref, out_hbm, damped_hbm, out_ref, damped_ref, sems
):
    stores = []
    rows = iota2((TOK, TOK), 0)
    cols = iota2((TOK, TOK), 1)
    same = (rows // BLOCK) == (cols // BLOCK)
    lower = same & (cols <= rows)
    upper = same & (cols >= rows)
    blocks = TOK // BLOCK
    for h in range(HEADS):
        lanes = slice(h * DK, (h + 1) * DK)
        closed = shut(logit_ref[:, lanes].astype(f32))
        extra = head_extra(extra_ref, h, 1)
        query = query_ref[:, lanes].astype(f32)
        value = value_ref[:, lanes]
        outs = [None] * blocks
        inner_sum = jnp.zeros((TOK, DK), f32)
        for d in range(2):
            seen = lower if d == 0 else upper
            keyed, decay = gate(closed, floor_ref[d : d + 1, lanes], extra)
            within = exact_sum(seen.astype(f32).astype(bf16), decay)
            damped = query * jnp.exp(within)
            grown = (keyed * jnp.exp(-within)).astype(bf16)
            damped16 = damped.astype(bf16)
            scores = jnp.where(seen, dot(damped16, grown, NT), 0.0).astype(bf16)
            inner_sum = inner_sum + dot(scores, value)
            state = None
            offset = jnp.zeros((1, DK), f32)
            for b in range(blocks) if d == 0 else reversed(range(blocks)):
                at = slice(b * BLOCK, (b + 1) * BLOCK)
                edge = (b + 1) * BLOCK - 1 if d == 0 else b * BLOCK
                total = within[edge : edge + 1]
                damped_ref[d, at, lanes] = (damped[at] * jnp.exp(offset)).astype(bf16)
                if state is not None:
                    cross = dot(damped16[at], state.astype(bf16), NT)
                    outs[b] = cross if outs[b] is None else outs[b] + cross
                offset = offset + total
                if b == (blocks - 1 if d == 0 else 0):
                    continue
                weighted = (keyed[at] * jnp.exp(total - within[at])).astype(bf16)
                added = dot(value[at], weighted, TN)
                state = added if state is None else state * jnp.exp(total) + added
        for b in range(blocks):
            at = slice(b * BLOCK, (b + 1) * BLOCK)
            out_ref[at, lanes] = inner_sum[at] if outs[b] is None else inner_sum[at] + outs[b]
        stores.append(pltpu.make_async_copy(out_ref.at[:, lanes], out_hbm.at[:, lanes], sems.at[h, 0]))
        stores.append(
            pltpu.make_async_copy(damped_ref.at[:, :, lanes], damped_hbm.at[:, :, lanes], sems.at[h, 1])
        )
        for store in stores[-2:]:
            store.start()
    for store in stores:
        store.wait()


def scan_kernel(got_ref, out_ref):
    d = lax.axis_index("sp_1") // HEADS
    carried = jnp.zeros((DK, DK), f32)
    for k in range(SEQ_DEV):
        j = jnp.where(d == 0, k, SEQ_DEV - 1 - k)
        out_ref[j] = carried.astype(bf16)
        if k < SEQ_DEV - 1:
            decay = got_ref[j, DK:STATE_ROWS, :][0:1].astype(f32)
            carried = carried * decay + got_ref[j, 0:DK, :].astype(f32)


def unpack_rope(rope_ref, ref):
    even = lax.axis_index("sp_1") % 2 == 0
    for j in range(SEQ_DEV):
        one = ref[j, 128:KV_ROWS, :].astype(f32)
        two = ref[j, KV_ROWS + 128 : 2 * KV_ROWS, :].astype(f32)
        rope_ref[j * 128 : j * 128 + 128, :] = jnp.transpose(
            jnp.concatenate(
                [
                    jnp.zeros((NOPE, 128), f32),
                    jnp.where(even, one, two),
                    jnp.where(even, two, one),
                    jnp.zeros((32, 128), f32),
                ],
                axis=0,
            )
        ).astype(bf16)


def expand(ex_ref, ref, up_ref):
    columns = pl.ds(pl.multiple_of(lax.axis_index("tp") * HEADS * 128, HEADS * 128), HEADS * 128)
    odd = lax.axis_index("sp_1") % 2
    up = jnp.concatenate(
        [up_ref[pl.ds(pl.multiple_of(p * 128, 128), 128), columns] for p in (odd, 1 - odd)], axis=0
    )
    for j in range(SEQ_DEV):
        lat = jnp.concatenate([ref[j, 0:128, :], ref[j, KV_ROWS : KV_ROWS + 128, :]], axis=1)
        ex_ref[j * 128 : j * 128 + 128, :] = dot(lat, up).astype(bf16)


def expand_kernel(pair_ref, up_ref, ex_ref, rope_ref):
    unpack_rope(rope_ref, pair_ref)
    expand(ex_ref, pair_ref, up_ref)


def attend_kernel(
    query_ref, other_ref, ex_mine_ref, rope_mine_ref, up_ref, cos_ref, sin_ref, local_hbm, damped_hbm,
    gain_hbm,
    out_ref, lw_ref, local_ref, damped_ref, gain_ref,
    ex_ref, rope_ref, sems,
):
    loads = start_all(
        sems, [(local_hbm, local_ref), (damped_hbm, damped_ref), (gain_hbm, gain_ref)]
    )
    unpack_rope(rope_ref, other_ref)
    expand(ex_ref, other_ref, up_ref)
    spot = pl.ds(pl.multiple_of(lax.axis_index("sp_1") * TOK, TOK), TOK)
    cos, sin = cos_ref[:, spot], sin_ref[:, spot]
    nothing = jnp.zeros((NOPE, TOK), f32)
    cos_table = jnp.transpose(jnp.concatenate([nothing + 1.0, cos, cos, nothing[:32]], axis=0))
    sin_table = jnp.transpose(jnp.concatenate([nothing, -sin, sin, nothing[:32]], axis=0))
    log_weights = []
    lane = iota2((TOK, 128), 1)
    q_blocks = [query_ref[:, 128 * i : 128 * i + 128].astype(f32) for i in range(3)]
    key_lane = iota2((SEQ_DEV * HALF, 128), 1)
    for h in range(HEADS):
        lanes = slice(h * 128, (h + 1) * 128)
        if h == 0:
            q = q_blocks[0]
        elif h == 1:
            q = jnp.where(lane < 32, pltpu.roll(q_blocks[0], 32, 1), pltpu.roll(q_blocks[1], 32, 1))
        elif h == 2:
            q = jnp.where(lane < 64, pltpu.roll(q_blocks[1], 64, 1), pltpu.roll(q_blocks[2], 64, 1))
        else:
            q = pltpu.roll(q_blocks[2], 96, 1)
        q = rotated(q, cos_table, sin_table).astype(bf16)
        parts = []
        for ex_part, rope_part in ((ex_mine_ref, rope_mine_ref), (ex_ref, rope_ref)):
            ex = ex_part[:, lanes]
            parts.append((ex, dot(q, jnp.where(key_lane < NOPE, ex, rope_part[...]), NT)))
        peak = jnp.maximum(
            jnp.max(parts[0][1], axis=1, keepdims=True), jnp.max(parts[1][1], axis=1, keepdims=True)
        )
        total, mixed = 0.0, 0.0
        for ex, scores in parts:
            weights = jnp.exp2((scores - peak) * (SCALE * LOG2E))
            total = total + jnp.sum(weights, axis=1, keepdims=True)
            mixed = mixed + dot(weights.astype(bf16), ex)
        mixed = mixed / total
        log_weights.append(jnp.broadcast_to(peak * SCALE + jnp.log(total), (TOK, 32)))
        if h % 2 == 0:
            kept = pltpu.roll(mixed, 64, 1)
        else:
            out_ref[:, (h // 2) * 128 : (h // 2) * 128 + 128] = jnp.where(
                lane < 64, kept, mixed
            ).astype(bf16)
    turned = jnp.transpose(jnp.concatenate(log_weights, axis=1))
    for h in range(HEADS):
        lw_ref[h : h + 1, :] = turned[32 * h : 32 * h + 1]
    for load in loads:
        load.wait()


def finish_kernel(
    local_ref, damped_ref, state_ref, gain_ref, att_ref, far_ref, top_hbm, low_hbm, left_hbm, right_hbm,
    send_ref, keep_ref,
    weight_ref, act_ref, sems,
):
    tp, column = lax.axis_index("tp"), lax.axis_index("fs")
    loads = start_all(
        sems,
        [
            (top_hbm, weight_ref.at[0, 0:512, :]),
            (low_hbm, weight_ref.at[0, 512:768, :]),
            (left_hbm, weight_ref.at[1]),
            (right_hbm, weight_ref.at[2]),
        ],
    )
    for part in range(2):
        start = jnp.where(tp == part, HALF, 0)
        at = pl.ds(pl.multiple_of(start, HALF), HALF)
        to = slice(part * HALF, (part + 1) * HALF)
        for h in range(HEADS):
            lanes = slice(h * DK, (h + 1) * DK)
            damped = jnp.concatenate([damped_ref[0, at, lanes], damped_ref[1, at, lanes]], axis=1)
            state = jnp.concatenate([state_ref[h], state_ref[HEADS + h]], axis=1)
            o = local_ref[at, lanes] + dot(damped, state, NT)
            mean = jnp.sum(o * o, axis=1, keepdims=True) * (1.0 / DK)
            act_ref[to, lanes] = (o * lax.rsqrt(mean + EPS) * gain_ref[:, lanes]).astype(bf16)
        act_ref[to, HEADS * DK :] = att_ref[at, :]
    act = act_ref[...]
    for i in range(4):
        for load in ((), loads[:2], loads[2:3], loads[3:])[i]:
            load.wait()
        got = dot(act, far_ref[...] if i == 0 else weight_ref[i - 1]).astype(bf16)
        lanes = pl.ds(pl.multiple_of(((column + (2, 0, 3, 1)[i]) % 4) * 512, 512), 512)
        send_ref[:, lanes] = got[:HALF]
        keep_ref[:, lanes] = got[HALF:]


SPACES = {"v": pltpu.VMEM, "h": pltpu.HBM}


def call(kernel, ins, outs, *args, scratch=(), flops=0, mib=16):
    args = [
        pltpu.with_memory_space_constraint(a, pltpu.HBM) if c == "h" else a for c, a in zip(ins, args)
    ]
    many = isinstance(outs, tuple)
    listed = outs if many else (outs,)
    spaces = [pltpu.HBM if type(o) is HbmOut else pltpu.VMEM for o in listed]
    shapes = tuple(
        pltpu.HBM(o.dims, o.dtype)
        if type(o) is HbmOut
        else o
        for o in listed
    )
    specs = tuple(pl.BlockSpec(memory_space=space) for space in spaces)
    return pl.pallas_call(
        kernel,
        out_shape=shapes if many else shapes[0],
        in_specs=[pl.BlockSpec(memory_space=SPACES[c]) for c in ins],
        out_specs=specs if many else specs[0],
        scratch_shapes=list(scratch),
        cost_estimate=pl.CostEstimate(flops=flops, bytes_accessed=1 << 20, transcendentals=0),
        compiler_params=pltpu.CompilerParams(vmem_limit_bytes=mib << 20),
    )(*args)


class HbmOut:
    def __init__(self, dims, dtype):
        self.dims, self.dtype = dims, dtype


def shape(dims, dtype):
    return jax.ShapeDtypeStruct(dims, dtype)


NEXT = [(i, (i + (1 if i % 2 else 7)) % 8) for i in range(8)]


def ring(n, step):
    return [(i, (i + step) % n) for i in range(n)]


def exchange(value):
    return lax.all_to_all(value, "sp_1", split_axis=0, concat_axis=0, tiled=True)


def local(
    recurrent_query,
    forget_logits,
    recurrent_value,
    forget_floor,
    extra_log_decay,
    recurrent_norm_gain,
    attention_query,
    latent,
    rotary_key,
    latent_norm_gain,
    latent_up_weight,
    recurrent_output_weight,
    attention_output_weight,
):
    cos_table, sin_table = rotary_tables()
    logits, values = forget_logits[0], recurrent_value[0]
    extra = jnp.swapaxes(extra_log_decay[0], 0, 1)

    sent = call(
        send_kernel,
        "h" * 9,
        HbmOut((SEQ_DEV, CHUNK_ROWS, DK), bf16),
        logits, values, forget_floor, extra, latent[0], latent_norm_gain.reshape(1, RANK),
        jnp.swapaxes(rotary_key[0], 0, 1), cos_table, sin_table,
        scratch=(
            pltpu.VMEM((TOK, HEADS * DK), bf16),
            pltpu.VMEM((TOK, HEADS * DK), bf16),
            pltpu.VMEM((2, HEADS * DK), f32),
            pltpu.VMEM((HEADS, TOK), f32),
            pltpu.VMEM((HALF, RANK), bf16),
            pltpu.VMEM((1, RANK), f32),
            pltpu.VMEM((ROPE, TOK), bf16),
            pltpu.VMEM((16, HALF), f32),
            pltpu.VMEM((16, HALF), f32),
            pltpu.VMEM((2 * HEADS, STATE_ROWS, DK), bf16),
            pltpu.VMEM((2, KV_ROWS, DK), bf16),
            pltpu.SemaphoreType.DMA((9,)),
            pltpu.SemaphoreType.DMA((SEQ_DEV,)),
            pltpu.SemaphoreType.DMA((2 * HEADS,)),
        ),
        flops=1 << 29, mib=14,
    )
    got = exchange(sent)

    weights = jnp.concatenate([recurrent_output_weight, attention_output_weight], axis=0)
    from_left = lax.ppermute(weights, "fs", ring(4, 1))
    from_right = lax.ppermute(weights, "fs", ring(4, -1))
    far = lax.ppermute(weights, "fs", ring(4, 2))

    local_out, damped = call(
        local_kernel,
        "vvvvv",
        (HbmOut((TOK, HEADS * DK), f32), HbmOut((2, TOK, HEADS * DK), bf16)),
        recurrent_query[0], logits, values, forget_floor, extra,
        scratch=(
            pltpu.VMEM((TOK, HEADS * DK), f32),
            pltpu.VMEM((2, TOK, HEADS * DK), bf16),
            pltpu.SemaphoreType.DMA((HEADS, 2)),
        ),
        flops=1 << 30, mib=14,
    )

    scanned = call(
        scan_kernel, "v", shape((SEQ_DEV, DK, DK), bf16), got,
        flops=1 << 26, mib=8,
    )
    states = exchange(scanned)

    mine = got[:, STATE_ROWS:]
    pair = jnp.concatenate([mine, lax.ppermute(mine, "sp_1", NEXT)], axis=1)
    other = lax.ppermute(pair, "tp", [(0, 1), (1, 0)])
    keys = SEQ_DEV * HALF
    ex_mine, rope_mine = call(
        expand_kernel, "vv",
        (shape((keys, HEADS * 128), bf16), shape((keys, 128), bf16)),
        pair, latent_up_weight,
        flops=1 << 28, mib=12,
    )
    attended, log_weight, local_out, damped, gain = call(
        attend_kernel,
        "v" * 7 + "hhh",
        (
            shape((TOK, HEADS * 64), bf16),
            shape((HEADS, TOK), f32),
            shape((TOK, HEADS * DK), f32),
            shape((2, TOK, HEADS * DK), bf16),
            shape((1, HEADS * DK), f32),
        ),
        attention_query[0], other, ex_mine, rope_mine, latent_up_weight, cos_table, sin_table,
        local_out, damped, recurrent_norm_gain.reshape(1, HEADS * DK),
        scratch=(
            pltpu.VMEM((keys, HEADS * 128), bf16),
            pltpu.VMEM((keys, 128), bf16),
            pltpu.SemaphoreType.DMA((3,)),
        ),
        flops=1 << 31, mib=24,
    )

    send, keep = call(
        finish_kernel,
        "v" * 6 + "hhhh",
        (shape((HALF, 2048), bf16), shape((HALF, 2048), bf16)),
        local_out, damped, states, gain, attended, far,
        recurrent_output_weight, attention_output_weight, from_left, from_right,
        scratch=(
            pltpu.VMEM((3, 768, 512), bf16),
            pltpu.VMEM((TOK, 768), bf16),
            pltpu.SemaphoreType.DMA((4,)),
        ),
        flops=1 << 30, mib=16,
    )
    arrived = lax.ppermute(send, "tp", [(0, 1), (1, 0)])
    mixed = (keep.astype(f32) + arrived.astype(f32)).astype(bf16)
    return mixed[None], jnp.swapaxes(log_weight, 0, 1)[None]


def rotary_tables():
    inverse = np.power(
        np.float32(ROPE_BASE), -np.arange(16, dtype=np.float32) / np.float32(16), dtype=np.float32
    )
    angle = inverse[:, None] * np.arange(SEQ_DEV * TOK, dtype=np.float32)[None, :]
    angle = angle.astype(np.float64)
    return np.cos(angle).astype(np.float32), np.sin(angle).astype(np.float32)


def solution(mesh):
    torus = Mesh(
        mesh.devices.reshape(8, 8, mesh.shape["fs"], mesh.shape["tp"]), ("sp_0", "sp_1", "fs", "tp")
    )
    in_specs = (
        P("fs", SP, "tp"),
        P("fs", SP, "tp"),
        P("fs", SP, "tp"),
        P(None, "tp"),
        P("fs", SP, "tp"),
        P("tp"),
        P("fs", SP, "tp"),
        P("fs", SP, None),
        P("fs", SP, None),
        P(),
        P(),
        P("tp", "fs"),
        P("tp", "fs"),
    )
    out_specs = (P("fs", SP_TP, None), P("fs", SP, "tp"))
    return jax.shard_map(local, mesh=torus, in_specs=in_specs, out_specs=out_specs, check_vma=False)
```
